32 devices in a mesh: sp: 16 (over z, y, x), tp: 2 (over core).
Axes of the slice: x: 2, y: 2, z: 4, core: 2. Of those that a mesh axis runs over, the one named last changes fastest.
Arguments:
- conv_value: bfloat16 [4096, 1024], P('sp', 'tp'), may hold values from -6 to 6
- conv_gate: bfloat16 [4096, 1024], P('sp', 'tp'), may hold values from -6 to 6
- taps: bfloat16 [31, 1024], P(None, 'tp'), may hold values from -1 to 1
- doc_ids: int32 [4096], P('sp'), may hold values from 0 to 3, never falling along the last dimension, each value on 1 to 2048 neighbouring positions
- gn_gain: float32 [1024], P('tp'), may hold values from 0.1 to 1.9
- gn_shift: float32 [1024], P('tp'), may hold values from -3 to 3
- conv_out: bfloat16 [1024, 2048], replicated, may hold values from -0.1875 to 0.1875
- residual: bfloat16 [4096, 2048], P(('sp', 'tp')), may hold values from -6 to 6
- norm_gain: float32 [2048], replicated, may hold values from 0.1 to 1.9
- routes: int32 [4096, 2], P(('sp', 'tp')), may hold values from 0 to 31, as said below
- route_weight: float32 [4096, 2], P(('sp', 'tp')), may hold values from 0.3 to 1.2
- expert_gate: bfloat16 [32, 2048, 512], P(('sp', 'tp')), may hold values from -0.125 to 0.125
- expert_up: bfloat16 [32, 2048, 512], P(('sp', 'tp')), may hold values from -0.125 to 0.125
- expert_down: bfloat16 [32, 512, 2048], P(('sp', 'tp')), may hold values from -0.25 to 0.25
- shared_gate: bfloat16 [2048, 512], replicated, may hold values from -0.125 to 0.125
- shared_up: bfloat16 [2048, 512], replicated, may hold values from -0.125 to 0.125
- shared_down: bfloat16 [512, 2048], replicated, may hold values from -0.25 to 0.25
Outputs:
- layer_out: bfloat16 [4096, 2048], P(('sp', 'tp'))
The draws below stay inside these ranges and needn't reach their ends.
Inputs may be any that keep to these rules, and one draw needn't show every extreme that they name: `routes`: each row names 2 different experts. The rows of one device name each expert at most 16 times, and one expert, the same for every device, exactly 16 times. `doc_ids`: numbers never fall from one position to the next.
All inputs are finite; a program needn't handle non-finite values.
Results may differ from the reference program's by a relative error of at most 0.014.
Values may be sent and summed in bfloat16 or wider, within the bound.
A program may use at most 128 MiB of HBM per device.

```python
import math
import jax
import jax.numpy as jnp
import numpy as np
from jax import lax

D = 2048
CONV_DIM = 1024
GROUPS = 8
WIDTH = 31
EXPERT_DIM = 512
SHARED_DIM = 512
TOP_K = 2
TOK_SP = 256
TOK_DEV = 128
TOKENS = 4096
EXPERTS = 32
CAP = 16
DOCS = 4


def draw_routes(key, part):
    blocks = TOKENS // TOK_DEV
    pairs = EXPERTS // 2
    key_order = jax.random.fold_in(key, 11)
    key_tilt = jax.random.fold_in(key, 12)
    key_noise = jax.random.fold_in(key, 13)
    key_rows = jax.random.fold_in(key, 14)
    order = jax.random.permutation(key_order, EXPERTS).astype(jnp.int32)
    tilt = jax.random.randint(key_tilt, (pairs,), 0, CAP + 1)
    noise = jax.random.randint(key_noise, (blocks, pairs), -(CAP // 4), CAP // 4 + 1)
    first = jnp.clip(tilt[None, :] + noise, 0, CAP)
    first = first.at[:, 0].set(CAP)
    pair_counts = jnp.stack([first, CAP - first], axis=2).reshape(blocks, EXPERTS)
    counts = jnp.zeros((blocks, EXPERTS), jnp.int32).at[:, order].set(pair_counts.astype(jnp.int32))
    cumulative = jnp.cumsum(counts, axis=1).astype(jnp.int32)
    positions = jnp.arange(TOK_DEV * TOP_K, dtype=jnp.int32)
    expert_of = jax.vmap(lambda row: jnp.searchsorted(row, positions, side='right'))(cumulative).astype(jnp.int32)
    slots = expert_of.reshape(blocks, TOP_K, TOK_DEV).transpose(0, 2, 1)
    row_keys = jax.random.split(key_rows, blocks)
    shuffles = jax.vmap(lambda one_key: jax.random.permutation(one_key, TOK_DEV))(row_keys).astype(jnp.int32)
    shuffles = jnp.broadcast_to(shuffles[:, :, None], (blocks, TOK_DEV, TOP_K))
    shuffled = jnp.take_along_axis(slots, shuffles, axis=1)
    return shuffled.reshape(TOKENS, TOP_K).astype(jnp.int32)


def level_of(key, extent, shards, low, high):
    loudness = 1.0
    for dim, parts in shards:
        draws = jax.random.uniform(jax.random.fold_in(jax.random.fold_in(key, 6), dim), (parts,), jnp.float32, low / len(shards), high / len(shards))
        loudness = loudness * jnp.repeat(jnp.exp(draws), extent[dim] // parts).reshape((-1,) + (1,) * (len(extent) - 1 - dim))
    return loudness


def length_profile(count, total, reach, slope):
    weights = [(1 << 20) // math.isqrt(rank ** slope) + 1 for rank in range(2, count + 1)]
    rest, holding = total - reach - (count - 1), [1] * (count - 1)
    while rest > 0:
        candidates = [i for i in range(count - 1) if holding[i] < reach]
        pool, left = sum([weights[i] for i in candidates]), rest
        for i in candidates:
            more = min(reach - holding[i], max(1, left * weights[i] // pool), rest)
            holding[i] = holding[i] + more
            rest = rest - more
    return np.array([reach] + holding)


def uneven_parts(own_key, amount, total, bound, lean):
    if amount == 2:
        one = jax.random.randint(own_key, (), max(1, total - bound), min(bound, total - 1) + 1)
        return jnp.stack([one, total - one])
    sizes = jnp.asarray(length_profile(amount, total, bound, lean), jnp.int32)
    couples = (amount - 1) // 2
    giver, taker = sizes[1:1 + 2 * couples:2], sizes[2:2 + 2 * couples:2]
    room = jnp.minimum(giver - 1, bound - taker)
    moved = jax.random.randint(jax.random.fold_in(own_key, 1), (couples,), 0, 1 << 20) % (room + 1)
    sizes = sizes.at[1:1 + 2 * couples:2].set(giver - moved).at[2:2 + 2 * couples:2].set(taker + moved)
    return sizes[jax.random.permutation(jax.random.fold_in(own_key, 2), amount)]


def normal_values(own_key, dims, scale, most, cuts=(), kind=jnp.bfloat16):
    array = scale * jax.random.normal(own_key, dims, jnp.float32)
    if cuts:
        array = array * level_of(own_key, dims, cuts, -0.22, 0.18)
    return jnp.clip(array, -most, most).astype(kind)


def setup_inputs(seed: int = 0) -> dict:
    arg_keys = jax.random.split(jax.random.key(seed), 18)
    return {
        "conv_value": normal_values(arg_keys[0], (TOKENS, CONV_DIM), 1.0, 6.0, ((0, 16), (1, 2))),
        "conv_gate": normal_values(arg_keys[1], (TOKENS, CONV_DIM), 1.0, 6.0, ((0, 16), (1, 2))),
        "taps": normal_values(arg_keys[2], (WIDTH, CONV_DIM), WIDTH ** -0.5, 1.0, ((1, 2),)),
        "doc_ids": jnp.searchsorted(jnp.cumsum(uneven_parts(arg_keys[3], DOCS, TOKENS, 8 * TOK_SP, 1)), jnp.arange(TOKENS), side="right").astype(jnp.int32),
        "gn_gain": jnp.clip(1.0 + 0.18 * jax.random.normal(arg_keys[4], (CONV_DIM,), jnp.float32), 0.1, 1.9),
        "gn_shift": normal_values(arg_keys[5], (CONV_DIM,), 0.5, 3.0, ((0, 2),), jnp.float32),
        "conv_out": normal_values(arg_keys[6], (CONV_DIM, D), CONV_DIM ** -0.5, 0.1875),
        "residual": normal_values(arg_keys[7], (TOKENS, D), 1.0, 6.0, ((0, 32),)),
        "norm_gain": jnp.clip(1.0 + 0.18 * jax.random.normal(arg_keys[8], (D,), jnp.float32), 0.1, 1.9),
        "routes": draw_routes(jax.random.fold_in(arg_keys[17], 71), 0),
        "route_weight": jnp.clip(0.3 + 0.90000004 * jax.random.uniform(arg_keys[10], (TOKENS, TOP_K), jnp.float32) ** level_of(arg_keys[10], (TOKENS, TOP_K), ((0, 32),), -0.2, 0.2), 0.3, 1.2),
        "expert_gate": normal_values(arg_keys[11], (EXPERTS, D, EXPERT_DIM), D ** -0.5, 0.125, ((0, 32),)),
        "expert_up": normal_values(arg_keys[12], (EXPERTS, D, EXPERT_DIM), D ** -0.5, 0.125, ((0, 32),)),
        "expert_down": normal_values(arg_keys[13], (EXPERTS, EXPERT_DIM, D), EXPERT_DIM ** -0.5, 0.25, ((0, 32),)),
        "shared_gate": normal_values(arg_keys[14], (D, SHARED_DIM), D ** -0.5, 0.125),
        "shared_up": normal_values(arg_keys[15], (D, SHARED_DIM), D ** -0.5, 0.125),
        "shared_down": normal_values(arg_keys[16], (SHARED_DIM, D), SHARED_DIM ** -0.5, 0.25),
    }


epsilon = 1e-06

def route_rows(normed, routes, route_weight, expert_gate, expert_up, expert_down):
    blocks = TOKENS // TOK_DEV
    flat_routes = routes.reshape(blocks, TOK_DEV * TOP_K).astype(jnp.int32)
    onehot = (flat_routes[:, :, None] == jnp.arange(EXPERTS, dtype=jnp.int32)[None, None, :]).astype(jnp.int32)
    slot_index = (lax.optimization_barrier(jnp.sum(jnp.cumsum(onehot, axis=1) * onehot, axis=2)) - 1).astype(jnp.int32)
    block_index = jnp.broadcast_to(jnp.arange(blocks, dtype=jnp.int32)[:, None], flat_routes.shape)
    row_index = (block_index * TOK_DEV + jnp.arange(TOK_DEV * TOP_K, dtype=jnp.int32)[None, :] // TOP_K).astype(jnp.int32)
    slot_table = jnp.full((EXPERTS, blocks, CAP), TOKENS, jnp.int32).at[flat_routes, block_index, slot_index].set(row_index)
    weight_table = jnp.zeros((EXPERTS, blocks, CAP), jnp.float32).at[flat_routes, block_index, slot_index].set(route_weight.reshape(blocks, TOK_DEV * TOP_K).astype(jnp.float32))
    padded_rows = jnp.concatenate([normed, jnp.zeros((1, D), normed.dtype)], axis=0)

    def one_expert(routed_sum, pieces):
        table_rows, table_weights, gate_weight, up_weight, down_weight = pieces
        expert_rows = padded_rows[table_rows]
        gate_part = jnp.dot(expert_rows, gate_weight, preferred_element_type=jnp.float32)
        up_part = jnp.dot(expert_rows, up_weight, preferred_element_type=jnp.float32)
        hidden = (jax.nn.silu(gate_part) * up_part).astype(jnp.bfloat16)
        result = jnp.dot(hidden, down_weight, preferred_element_type=jnp.float32).astype(jnp.bfloat16)
        routed_sum = routed_sum.at[table_rows].add(table_weights[:, None] * result.astype(jnp.float32), mode='drop')
        return (routed_sum, None)
    routed, _ = lax.scan(one_expert, jnp.zeros((TOKENS, D), jnp.float32), (slot_table.reshape(EXPERTS, blocks * CAP), weight_table.reshape(EXPERTS, blocks * CAP), expert_gate, expert_up, expert_down))
    return routed

def reference(conv_value, conv_gate, taps, doc_ids, gn_gain, gn_shift, conv_out, residual, norm_gain, routes, route_weight, expert_gate, expert_up, expert_down, shared_gate, shared_up, shared_down):
    glu = (conv_value.astype(jnp.float32) * jax.nn.sigmoid(conv_gate.astype(jnp.float32))).astype(jnp.bfloat16)
    padded_glu = jnp.pad(glu, ((WIDTH - 1, 0), (0, 0)))
    padded_ids = jnp.pad(doc_ids, (WIDTH - 1, 0), constant_values=-1)
    conv_sum = jnp.zeros((TOKENS, CONV_DIM), jnp.float32)
    for offset in range(WIDTH):
        same_doc = (padded_ids[offset:offset + TOKENS] == doc_ids)[:, None]
        tap_term = taps[offset].astype(jnp.float32)[None, :] * padded_glu[offset:offset + TOKENS].astype(jnp.float32)
        conv_sum = conv_sum + jnp.where(same_doc, tap_term, 0.0)
    grouped = conv_sum.reshape(TOKENS, GROUPS, CONV_DIM // GROUPS)
    group_mean = lax.optimization_barrier(jnp.mean(grouped, axis=-1, keepdims=True))
    centered = grouped - group_mean
    group_var = lax.optimization_barrier(jnp.mean(centered * centered, axis=-1, keepdims=True))
    normalized = (centered * lax.rsqrt(group_var + epsilon)).reshape(TOKENS, CONV_DIM)
    conv_act = jax.nn.silu(normalized * gn_gain + gn_shift).astype(jnp.bfloat16)
    projected = jnp.dot(conv_act, conv_out, preferred_element_type=jnp.float32)
    stream = (residual.astype(jnp.float32) + projected).astype(jnp.bfloat16)
    stream_wide = stream.astype(jnp.float32)
    normed = (stream_wide * lax.rsqrt(lax.optimization_barrier(jnp.mean(stream_wide * stream_wide, axis=-1, keepdims=True)) + epsilon) * norm_gain).astype(jnp.bfloat16)
    shared_hidden = (jax.nn.silu(jnp.dot(normed, shared_gate, preferred_element_type=jnp.float32)) * jnp.dot(normed, shared_up, preferred_element_type=jnp.float32)).astype(jnp.bfloat16)
    shared_out = jnp.dot(shared_hidden, shared_down, preferred_element_type=jnp.float32)
    routed = route_rows(normed, routes, route_weight, expert_gate, expert_up, expert_down)
    return (stream_wide + shared_out + routed).astype(jnp.bfloat16)
```

```python
import functools

import jax
import jax.numpy as jnp
from jax import lax
from jax.experimental import pallas as pl
from jax.experimental.pallas import tpu as pltpu
from jax.sharding import PartitionSpec as P

GROUPS = 8


epsilon = 1e-06


def from_behind(x, axis, by):
    peers = lax.axis_size(axis)
    pairs = [(i, i + by) for i in range(peers) if 0 <= i + by < peers]
    return lax.ppermute(x, axis, pairs)


def per_device(
    conv_value,
    conv_gate,
    taps,
    doc_ids,
    gn_gain,
    gn_shift,
    conv_out,
    residual,
    norm_gain,
    routes,
    route_weight,
    expert_gate,
    expert_up,
    expert_down,
    shared_gate,
    shared_up,
    shared_down,
):
    position_count, channel_count = conv_value.shape
    kernel_width = taps.shape[0]
    model_width = residual.shape[1]
    glu_out = (
        conv_value.astype(jnp.float32) * jax.nn.sigmoid(conv_gate.astype(jnp.float32))
    ).astype(jnp.bfloat16)
    rim_start = position_count - kernel_width + 1
    edge_glu, edge_ids = from_behind((glu_out[rim_start:], doc_ids[rim_start:]), "sp", 1)
    longer_glu = jnp.concatenate([edge_glu, glu_out], axis=0)
    longer_ids = jnp.concatenate([edge_ids, doc_ids], axis=0)
    conv_sum = jnp.zeros((position_count, channel_count), jnp.float32)
    for offset in range(kernel_width):
        same_doc = (longer_ids[offset : offset + position_count] == doc_ids)[:, None]
        tap_term = taps[offset].astype(jnp.float32)[None, :] * longer_glu[
            offset : offset + position_count
        ].astype(jnp.float32)
        conv_sum = conv_sum + jnp.where(same_doc, tap_term, 0.0)
    core_split = lax.axis_size("tp")
    groups_here = GROUPS // core_split
    grouped = conv_sum.reshape(position_count, groups_here, channel_count // groups_here)
    group_mean = jnp.mean(grouped, axis=-1, keepdims=True)
    centered = grouped - group_mean
    group_var = jnp.mean(centered * centered, axis=-1, keepdims=True)
    normalized = (centered * lax.rsqrt(group_var + epsilon)).reshape(position_count, channel_count)
    conv_act = jax.nn.silu(normalized * gn_gain + gn_shift).astype(jnp.bfloat16)
    token_rows = lax.all_to_all(conv_act, "tp", split_axis=0, concat_axis=1, tiled=True)
    projected = jnp.dot(token_rows, conv_out, preferred_element_type=jnp.float32)
    stream = (residual.astype(jnp.float32) + projected).astype(jnp.bfloat16)
    stream_wide = stream.astype(jnp.float32)
    normed = (
        stream_wide
        * lax.rsqrt(jnp.mean(stream_wide * stream_wide, axis=-1, keepdims=True) + epsilon)
        * norm_gain
    ).astype(jnp.bfloat16)
    token_count, top_count = routes.shape
    sequence_split = lax.axis_size("sp")
    device_count = sequence_split * core_split
    local_experts = expert_gate.shape[0]
    experts = local_experts * device_count
    capacity = 2 * token_count * top_count // experts
    flat_routes = routes.reshape(-1)
    onehot = (flat_routes[:, None] == jnp.arange(experts, dtype=jnp.int32)[None, :]).astype(
        jnp.int32
    )
    slot_index = jnp.sum(jnp.cumsum(onehot, axis=0) * onehot, axis=1) - 1
    target = flat_routes * capacity + slot_index
    source = (
        jnp.full((experts * capacity,), token_count, jnp.int32)
        .at[target]
        .set(jnp.arange(token_count * top_count, dtype=jnp.int32) // top_count)
    )
    padded_rows = jnp.concatenate([normed, jnp.zeros((1, model_width), normed.dtype)], axis=0)
    outgoing = padded_rows[source]
    shared_hidden = (
        jax.nn.silu(jnp.dot(normed, shared_gate, preferred_element_type=jnp.float32))
        * jnp.dot(normed, shared_up, preferred_element_type=jnp.float32)
    ).astype(jnp.bfloat16)
    shared_out = jnp.dot(shared_hidden, shared_down, preferred_element_type=jnp.float32)
    parcel = outgoing.reshape(device_count, local_experts, capacity, model_width)
    arrived = lax.all_to_all(parcel, ("sp", "tp"), split_axis=0, concat_axis=0, tiled=True)
    expert_rows = arrived[:, 0].reshape(-1, model_width)
    gate_part = jnp.dot(expert_rows, expert_gate[0], preferred_element_type=jnp.float32)
    up_part = jnp.dot(expert_rows, expert_up[0], preferred_element_type=jnp.float32)
    hidden = (jax.nn.silu(gate_part) * up_part).astype(jnp.bfloat16)
    result = jnp.dot(hidden, expert_down[0], preferred_element_type=jnp.float32).astype(
        jnp.bfloat16
    )
    results = [result.reshape(arrived.shape[0], arrived.shape[2], model_width)]
    returned = lax.all_to_all(
        jnp.stack(results, axis=1), ("sp", "tp"), split_axis=0, concat_axis=0, tiled=True
    )
    picked = returned.reshape(experts * capacity, model_width)[target].reshape(
        token_count, top_count, model_width
    )
    routed = jnp.zeros((token_count, model_width), jnp.float32)
    for route_index in range(top_count):
        routed = routed + route_weight[:, route_index, None] * picked[:, route_index].astype(
            jnp.float32
        )
    return (stream_wide + shared_out + routed).astype(jnp.bfloat16)


F32 = jnp.float32
BF16 = jnp.bfloat16
MESH_ID = pl.DeviceIdType.MESH
HALO = 32
CHUNK = 32


def flip(index, bits):
    out, weight = index, 1
    while weight <= bits:
        if (bits // weight) % 2:
            out = out + weight * (1 - 2 * ((index // weight) % 2))
        weight *= 2
    return out


def silu(v):
    return v / (1.0 + jnp.exp(-v))


def fused_kernel(
    n_sp,
    n_tp,
    capacity,
    value_ref,
    gate_ref,
    taps_ref,
    ids_ref,
    gain_ref,
    shift_ref,
    resid_ref,
    ngain_ref,
    routes_ref,
    routes_t_ref,
    weight_ref,
    conv_out_hbm,
    eg_hbm,
    eu_hbm,
    ed_hbm,
    sg_hbm,
    su_hbm,
    sd_hbm,
    out_ref,
    glu_ext,
    ids_ext,
    tap_rows,
    halo_send,
    halo_recv,
    act,
    act_recv,
    normed_ref,
    base_ref,
    send_buf,
    arrived,
    result,
    returned,
    conv_out,
    eg,
    eu,
    ed,
    sg,
    su,
    sd,
    w_sem,
    halo_sem,
    act_sem,
    out_send,
    out_recv,
    back_send,
    back_recv,
    own_sem,
):
    n = n_sp * n_tp
    sp, tp = lax.axis_index("sp"), lax.axis_index("tp")
    me = sp * n_tp + tp
    rows, channels = value_ref.shape
    tokens, model = resid_ref.shape
    width = taps_ref.shape[0]
    group = glu_ext.shape[2]
    groups = channels // group

    def place(index):
        return (index // n_tp, index % n_tp)

    loads = [
        pltpu.make_async_copy(a, b, w_sem.at[i])
        for i, (a, b) in enumerate(
            [
                (conv_out_hbm, conv_out),
                (sg_hbm, sg),
                (su_hbm, su),
                (sd_hbm, sd),
                (eg_hbm, eg),
                (eu_hbm, eu),
                (ed_hbm, ed),
            ]
        )
    ]
    for load in loads:
        load.start()

    barrier = pltpu.get_barrier_semaphore()
    for j in range(1, n):
        pl.semaphore_signal(barrier, inc=1, device_id=place(flip(me, j)), device_id_type=MESH_ID)

    glu = (value_ref[...].astype(F32) * jax.nn.sigmoid(gate_ref[...].astype(F32))).astype(BF16)
    halo_send[...] = glu[rows - HALO :, :]
    for g in range(groups):
        glu_ext[g, pl.ds(HALO, rows), :] = glu[:, g * group : (g + 1) * group].astype(F32)
    ids_ext[pl.ds(HALO, rows), :] = ids_ref[...]
    tap_rows[pl.ds(0, width), :] = taps_ref[...].astype(F32)

    pl.semaphore_wait(barrier, n - 1)

    halo_copies = [
        pltpu.make_async_remote_copy(
            src_ref=halo_send,
            dst_ref=halo_recv,
            send_sem=halo_sem.at[0],
            recv_sem=halo_sem.at[1],
            device_id=(sp + 1, tp),
            device_id_type=MESH_ID,
        ),
        pltpu.make_async_remote_copy(
            src_ref=ids_ref.at[pl.ds(rows - HALO, HALO)],
            dst_ref=ids_ext.at[pl.ds(0, HALO)],
            send_sem=halo_sem.at[2],
            recv_sem=halo_sem.at[3],
            device_id=(sp + 1, tp),
            device_id_type=MESH_ID,
        ),
    ]

    @pl.when(sp < n_sp - 1)
    def _():
        for copy in halo_copies:
            copy.start()

    @pl.when(sp == 0)
    def _():
        glu_ext[:, pl.ds(0, HALO), :] = jnp.zeros((groups, HALO, group), F32)
        ids_ext[pl.ds(0, HALO), :] = jnp.full((HALO, ids_ext.shape[1]), -1, jnp.int32)

    slots = n * capacity
    expert_lane = lax.broadcasted_iota(jnp.int32, (tokens, n), 1)
    member = (
        (routes_ref[:, 0:1] == expert_lane).astype(F32)
        + (routes_ref[:, 1:2] == expert_lane).astype(F32)
    ).astype(BF16)
    tri_r = lax.broadcasted_iota(jnp.int32, (tokens, tokens), 0)
    tri_c = lax.broadcasted_iota(jnp.int32, (tokens, tokens), 1)
    slot_of = jnp.dot((tri_c < tri_r).astype(F32).astype(BF16), member, preferred_element_type=F32)
    spread = (
        (
            lax.broadcasted_iota(jnp.int32, (n, slots), 1) // capacity
            == lax.broadcasted_iota(jnp.int32, (n, slots), 0)
        )
        .astype(F32)
        .astype(BF16)
    )
    slot_wide = jnp.dot(slot_of.astype(BF16), spread, preferred_element_type=F32)
    lane = lax.broadcasted_iota(jnp.int32, (tokens, slots), 1)
    lane_expert = lane // capacity
    right_slot = slot_wide == (lane % capacity).astype(F32)
    weights = jnp.where(lane_expert == routes_ref[:, 0:1], weight_ref[:, 0:1], 0.0) + jnp.where(
        lane_expert == routes_ref[:, 1:2], weight_ref[:, 1:2], 0.0
    )
    weights = jnp.where(right_slot, weights, 0.0)
    w_high = weights.astype(BF16)
    w_low = (weights - w_high.astype(F32)).astype(BF16)

    expert_row = lax.broadcasted_iota(jnp.int32, (n, tokens), 0)
    member_t = (
        (routes_t_ref[0:1, :] == expert_row).astype(F32)
        + (routes_t_ref[1:2, :] == expert_row).astype(F32)
    ).astype(BF16)
    slot_t = jnp.dot(member_t, (tri_r < tri_c).astype(F32).astype(BF16), preferred_element_type=F32)
    spread_t = (
        (
            lax.broadcasted_iota(jnp.int32, (slots, n), 0) // capacity
            == lax.broadcasted_iota(jnp.int32, (slots, n), 1)
        )
        .astype(F32)
        .astype(BF16)
    )
    slot_tall = jnp.dot(spread_t, slot_t.astype(BF16), preferred_element_type=F32)
    member_tall = jnp.dot(spread_t, member_t, preferred_element_type=F32)
    row_slot = (lax.broadcasted_iota(jnp.int32, (slots, tokens), 0) % capacity).astype(F32)
    pick = jnp.where(slot_tall == row_slot, member_tall, 0.0).astype(BF16)

    @pl.when(sp > 0)
    def _():
        for copy in halo_copies:
            copy.wait_recv()
        for g in range(groups):
            glu_ext[g, pl.ds(0, HALO), :] = halo_recv[:, g * group : (g + 1) * group].astype(F32)

    @pl.when(sp < n_sp - 1)
    def _():
        for copy in halo_copies:
            copy.wait_send()

    def conv_block(start):
        def body(i, carry):
            r = pl.multiple_of(start + i * CHUNK, CHUNK)
            mine = ids_ref[pl.ds(r, CHUNK), :]
            sums = [jnp.zeros((CHUNK, group), F32) for _ in range(groups)]
            for tap in range(width):
                off = HALO - width + 1 + tap
                same = ids_ext[pl.ds(r + off, CHUNK), :] == mine
                for g in range(groups):
                    term = (
                        tap_rows[tap : tap + 1, g * group : (g + 1) * group]
                        * glu_ext[g, pl.ds(r + off, CHUNK), :]
                    )
                    sums[g] = sums[g] + jnp.where(same, term, 0.0)
            for g in range(groups):
                cols = slice(g * group, (g + 1) * group)
                centered = sums[g] - jnp.mean(sums[g], axis=-1, keepdims=True)
                var = jnp.mean(centered * centered, axis=-1, keepdims=True)
                v = centered * lax.rsqrt(var + epsilon) * gain_ref[:, cols] + shift_ref[:, cols]
                act[pl.ds(r, CHUNK), cols] = silu(v).astype(BF16)
            return carry

        lax.fori_loop(0, tokens // CHUNK, body, 0)

    other = (tp + 1) % n_tp
    theirs = pl.multiple_of(other * tokens, tokens)
    mine_at = pl.multiple_of(tp * tokens, tokens)
    conv_block(theirs)
    act_copy = pltpu.make_async_remote_copy(
        src_ref=act.at[pl.ds(theirs, tokens)],
        dst_ref=act_recv,
        send_sem=act_sem.at[0],
        recv_sem=act_sem.at[1],
        device_id=(sp, other),
        device_id_type=MESH_ID,
    )
    act_copy.start()
    conv_block(mine_at)
    loads[0].wait()
    half = channels
    projected = jnp.dot(
        act[pl.ds(mine_at, tokens), :],
        conv_out[pl.ds(pl.multiple_of(tp * half, half), half), :],
        preferred_element_type=F32,
    )
    act_copy.wait()
    projected = projected + jnp.dot(
        act_recv[...],
        conv_out[pl.ds(pl.multiple_of(other * half, half), half), :],
        preferred_element_type=F32,
    )
    stream = (resid_ref[...].astype(F32) + projected).astype(BF16).astype(F32)
    base_ref[...] = stream
    normed = (
        stream
        * lax.rsqrt(jnp.mean(stream * stream, axis=-1, keepdims=True) + epsilon)
        * ngain_ref[...]
    ).astype(BF16)
    normed_ref[...] = normed

    batches = BATCHES
    per = n // batches
    block = per * capacity

    def outgoing(index, peer):
        return pltpu.make_async_remote_copy(
            src_ref=send_buf.at[pl.ds(pl.multiple_of(peer * capacity, capacity), capacity)],
            dst_ref=arrived.at[pl.ds(pl.multiple_of(me * capacity, capacity), capacity)],
            send_sem=out_send.at[index],
            recv_sem=out_recv.at[index],
            device_id=place(peer),
            device_id_type=MESH_ID,
        )

    def incoming(index, peer):
        return pltpu.make_async_remote_copy(
            src_ref=send_buf.at[pl.ds(pl.multiple_of(me * capacity, capacity), capacity)],
            dst_ref=arrived.at[pl.ds(pl.multiple_of(peer * capacity, capacity), capacity)],
            send_sem=out_send.at[index],
            recv_sem=out_recv.at[index],
            device_id=place(peer),
            device_id_type=MESH_ID,
        )

    def homeward(index, peer):
        return pltpu.make_async_remote_copy(
            src_ref=result.at[pl.ds(pl.multiple_of(peer * capacity, capacity), capacity)],
            dst_ref=returned.at[pl.ds(pl.multiple_of(me * capacity, capacity), capacity)],
            send_sem=back_send.at[index],
            recv_sem=back_recv.at[index],
            device_id=place(peer),
            device_id_type=MESH_ID,
        )

    def coming_home(index, peer):
        return pltpu.make_async_remote_copy(
            src_ref=result.at[pl.ds(pl.multiple_of(me * capacity, capacity), capacity)],
            dst_ref=returned.at[pl.ds(pl.multiple_of(peer * capacity, capacity), capacity)],
            send_sem=back_send.at[index],
            recv_sem=back_recv.at[index],
            device_id=place(peer),
            device_id_type=MESH_ID,
        )

    send_buf[...] = jnp.dot(pick, normed, preferred_element_type=F32).astype(BF16)
    for j in range(n - 1, 0, -1):
        outgoing(j, flip(me, j)).start()
    own = pl.ds(pl.multiple_of(me * capacity, capacity), capacity)
    arrived[own, :] = send_buf[own, :]

    for load in loads[1:4]:
        load.wait()
    shared = (
        silu(jnp.dot(normed_ref[...], sg[...], preferred_element_type=F32))
        * jnp.dot(normed_ref[...], su[...], preferred_element_type=F32)
    ).astype(BF16)
    base_ref[...] += jnp.dot(shared, sd[...], preferred_element_type=F32)
    for load in loads[4:]:
        load.wait()

    for b in range(batches - 1, -1, -1):
        for low in range(per - 1, -1, -1):
            j = b * per + low
            if j:
                incoming(j, flip(me, j)).wait_recv()
        at = pl.ds(pl.multiple_of(flip(me // per, b) * block, block), block)
        x = arrived[at, :]
        hidden = (
            silu(jnp.dot(x, eg[0], preferred_element_type=F32))
            * jnp.dot(x, eu[0], preferred_element_type=F32)
        ).astype(BF16)
        result[at, :] = jnp.dot(hidden, ed[0], preferred_element_type=F32).astype(BF16)
        for low in range(per - 1, -1, -1):
            j = b * per + low
            if j:
                homeward(j, flip(me, j)).start()
    returned[own, :] = result[own, :]

    for j in range(n - 1, 0, -1):
        coming_home(j, flip(me, j)).wait_recv()
    back = returned[...]
    routed = jnp.dot(w_high, back, preferred_element_type=F32) + jnp.dot(
        w_low, back, preferred_element_type=F32
    )
    out_ref[...] = (base_ref[...] + routed).astype(BF16)
    for j in range(n - 1, 0, -1):
        outgoing(j, flip(me, j)).wait_send()
        homeward(j, flip(me, j)).wait_send()


def fused(
    conv_value,
    conv_gate,
    taps,
    doc_ids,
    gn_gain,
    gn_shift,
    conv_out,
    residual,
    norm_gain,
    routes,
    route_weight,
    expert_gate,
    expert_up,
    expert_down,
    shared_gate,
    shared_up,
    shared_down,
):
    n_sp, n_tp = lax.axis_size("sp"), lax.axis_size("tp")
    n = n_sp * n_tp
    rows, channels = conv_value.shape
    tokens, model = residual.shape
    capacity = 2 * tokens * routes.shape[1] // n
    group = channels * n_tp // GROUPS
    hidden = expert_gate.shape[2]
    slots = n * capacity
    vmem = pl.BlockSpec(memory_space=pltpu.VMEM)
    hbm = pl.BlockSpec(memory_space=pl.ANY)
    dma = pltpu.SemaphoreType.DMA
    ids = jnp.broadcast_to(doc_ids[:, None], (rows, group))
    return pl.pallas_call(
        functools.partial(fused_kernel, n_sp, n_tp, capacity),
        out_shape=jax.ShapeDtypeStruct((tokens, model), BF16),
        in_specs=[vmem] * 11 + [hbm] * 7,
        out_specs=vmem,
        scratch_shapes=[
            pltpu.VMEM((channels // group, rows + HALO, group), F32),
            pltpu.VMEM((rows + HALO, group), jnp.int32),
            pltpu.VMEM((taps.shape[0] + 1, channels), F32),
            pltpu.VMEM((HALO, channels), BF16),
            pltpu.VMEM((HALO, channels), BF16),
            pltpu.VMEM((rows, channels), BF16),
            pltpu.VMEM((tokens, channels), BF16),
            pltpu.VMEM((tokens, model), BF16),
            pltpu.VMEM((tokens, model), F32),
            pltpu.VMEM((slots, model), BF16),
            pltpu.VMEM((slots, model), BF16),
            pltpu.VMEM((slots, model), BF16),
            pltpu.VMEM((slots, model), BF16),
            pltpu.VMEM(conv_out.shape, BF16),
            pltpu.VMEM(expert_gate.shape, BF16),
            pltpu.VMEM(expert_up.shape, BF16),
            pltpu.VMEM(expert_down.shape, BF16),
            pltpu.VMEM(shared_gate.shape, BF16),
            pltpu.VMEM(shared_up.shape, BF16),
            pltpu.VMEM(shared_down.shape, BF16),
            dma((7,)),
            dma((4,)),
            dma((2,)),
            dma((n,)),
            dma((n,)),
            dma((n,)),
            dma((n,)),
            dma((2,)),
        ],
        compiler_params=pltpu.CompilerParams(
            collective_id=0, has_side_effects=True, vmem_limit_bytes=VMEM_LIMIT
        ),
    )(
        conv_value,
        conv_gate,
        taps,
        ids,
        gn_gain[None, :],
        gn_shift[None, :],
        residual,
        norm_gain[None, :],
        routes,
        routes.T,
        route_weight,
        conv_out,
        expert_gate,
        expert_up,
        expert_down,
        shared_gate,
        shared_up,
        shared_down,
    )


BATCHES = 4
VMEM_LIMIT = 58 * 1024 * 1024


def fits(mesh):
    n = mesh.size
    return n & (n - 1) == 0 and n <= 32 and mesh.shape["tp"] == 2


def solution(mesh):
    return jax.shard_map(
        fused if fits(mesh) else per_device,
        mesh=mesh,
        in_specs=(
            P("sp", "tp"),
            P("sp", "tp"),
            P(None, "tp"),
            P("sp"),
            P("tp"),
            P("tp"),
            P(),
            P(("sp", "tp"), None),
            P(),
            P(("sp", "tp"), None),
            P(("sp", "tp"), None),
            P(("sp", "tp"), None, None),
            P(("sp", "tp"), None, None),
            P(("sp", "tp"), None, None),
            P(),
            P(),
            P(),
        ),
        out_specs=P(("sp", "tp"), None),
        check_vma=False,
    )
```

```python
import functools

import jax
import jax.numpy as jnp
from jax import lax
from jax.experimental import pallas as pl
from jax.experimental.pallas import tpu as pltpu
from jax.sharding import PartitionSpec as P

GROUPS = 8


epsilon = 1e-06


def from_behind(x, axis, by):
    peers = lax.axis_size(axis)
    pairs = [(i, i + by) for i in range(peers) if 0 <= i + by < peers]
    return lax.ppermute(x, axis, pairs)


def per_device(
    conv_value,
    conv_gate,
    taps,
    doc_ids,
    gn_gain,
    gn_shift,
    conv_out,
    residual,
    norm_gain,
    routes,
    route_weight,
    expert_gate,
    expert_up,
    expert_down,
    shared_gate,
    shared_up,
    shared_down,
):
    position_count, channel_count = conv_value.shape
    kernel_width = taps.shape[0]
    model_width = residual.shape[1]
    glu_out = (
        conv_value.astype(jnp.float32) * jax.nn.sigmoid(conv_gate.astype(jnp.float32))
    ).astype(jnp.bfloat16)
    rim_start = position_count - kernel_width + 1
    edge_glu, edge_ids = from_behind((glu_out[rim_start:], doc_ids[rim_start:]), "sp", 1)
    longer_glu = jnp.concatenate([edge_glu, glu_out], axis=0)
    longer_ids = jnp.concatenate([edge_ids, doc_ids], axis=0)
    conv_sum = jnp.zeros((position_count, channel_count), jnp.float32)
    for offset in range(kernel_width):
        same_doc = (longer_ids[offset : offset + position_count] == doc_ids)[:, None]
        tap_term = taps[offset].astype(jnp.float32)[None, :] * longer_glu[
            offset : offset + position_count
        ].astype(jnp.float32)
        conv_sum = conv_sum + jnp.where(same_doc, tap_term, 0.0)
    core_split = lax.axis_size("tp")
    groups_here = GROUPS // core_split
    grouped = conv_sum.reshape(position_count, groups_here, channel_count // groups_here)
    group_mean = jnp.mean(grouped, axis=-1, keepdims=True)
    centered = grouped - group_mean
    group_var = jnp.mean(centered * centered, axis=-1, keepdims=True)
    normalized = (centered * lax.rsqrt(group_var + epsilon)).reshape(position_count, channel_count)
    conv_act = jax.nn.silu(normalized * gn_gain + gn_shift).astype(jnp.bfloat16)
    token_rows = lax.all_to_all(conv_act, "tp", split_axis=0, concat_axis=1, tiled=True)
    projected = jnp.dot(token_rows, conv_out, preferred_element_type=jnp.float32)
    stream = (residual.astype(jnp.float32) + projected).astype(jnp.bfloat16)
    stream_wide = stream.astype(jnp.float32)
    normed = (
        stream_wide
        * lax.rsqrt(jnp.mean(stream_wide * stream_wide, axis=-1, keepdims=True) + epsilon)
        * norm_gain
    ).astype(jnp.bfloat16)
    token_count, top_count = routes.shape
    sequence_split = lax.axis_size("sp")
    device_count = sequence_split * core_split
    local_experts = expert_gate.shape[0]
    experts = local_experts * device_count
    capacity = 2 * token_count * top_count // experts
    flat_routes = routes.reshape(-1)
    onehot = (flat_routes[:, None] == jnp.arange(experts, dtype=jnp.int32)[None, :]).astype(
        jnp.int32
    )
    slot_index = jnp.sum(jnp.cumsum(onehot, axis=0) * onehot, axis=1) - 1
    target = flat_routes * capacity + slot_index
    source = (
        jnp.full((experts * capacity,), token_count, jnp.int32)
        .at[target]
        .set(jnp.arange(token_count * top_count, dtype=jnp.int32) // top_count)
    )
    padded_rows = jnp.concatenate([normed, jnp.zeros((1, model_width), normed.dtype)], axis=0)
    outgoing = padded_rows[source]
    shared_hidden = (
        jax.nn.silu(jnp.dot(normed, shared_gate, preferred_element_type=jnp.float32))
        * jnp.dot(normed, shared_up, preferred_element_type=jnp.float32)
    ).astype(jnp.bfloat16)
    shared_out = jnp.dot(shared_hidden, shared_down, preferred_element_type=jnp.float32)
    parcel = outgoing.reshape(device_count, local_experts, capacity, model_width)
    arrived = lax.all_to_all(parcel, ("sp", "tp"), split_axis=0, concat_axis=0, tiled=True)
    expert_rows = arrived[:, 0].reshape(-1, model_width)
    gate_part = jnp.dot(expert_rows, expert_gate[0], preferred_element_type=jnp.float32)
    up_part = jnp.dot(expert_rows, expert_up[0], preferred_element_type=jnp.float32)
    hidden = (jax.nn.silu(gate_part) * up_part).astype(jnp.bfloat16)
    result = jnp.dot(hidden, expert_down[0], preferred_element_type=jnp.float32).astype(
        jnp.bfloat16
    )
    results = [result.reshape(arrived.shape[0], arrived.shape[2], model_width)]
    returned = lax.all_to_all(
        jnp.stack(results, axis=1), ("sp", "tp"), split_axis=0, concat_axis=0, tiled=True
    )
    picked = returned.reshape(experts * capacity, model_width)[target].reshape(
        token_count, top_count, model_width
    )
    routed = jnp.zeros((token_count, model_width), jnp.float32)
    for route_index in range(top_count):
        routed = routed + route_weight[:, route_index, None] * picked[:, route_index].astype(
            jnp.float32
        )
    return (stream_wide + shared_out + routed).astype(jnp.bfloat16)


F32 = jnp.float32
BF16 = jnp.bfloat16
MESH_ID = pl.DeviceIdType.MESH
HALO = 32
CHUNK = 32


def flip(index, bits):
    out, weight = index, 1
    while weight <= bits:
        if (bits // weight) % 2:
            out = out + weight * (1 - 2 * ((index // weight) % 2))
        weight *= 2
    return out


def silu(v):
    return v / (1.0 + jnp.exp(-v))


def fused_kernel(
    n_sp,
    n_tp,
    capacity,
    value_ref,
    gate_ref,
    taps_ref,
    ids_ref,
    gain_ref,
    shift_ref,
    resid_ref,
    ngain_ref,
    routes_ref,
    weight_ref,
    conv_out_hbm,
    eg_hbm,
    eu_hbm,
    ed_hbm,
    sg_hbm,
    su_hbm,
    sd_hbm,
    out_ref,
    glu_ext,
    ids_ext,
    tap_rows,
    halo_send,
    halo_recv,
    act,
    act_recv,
    normed_ref,
    base_ref,
    far_tokens,
    far_routes,
    far_weight,
    ids_here,
    send_own,
    send_far,
    arrived,
    result,
    returned,
    relayed,
    part_send,
    part_recv,
    conv_out,
    eg,
    eu,
    ed,
    sg,
    su,
    sd,
    w_sem,
    halo_sem,
    act_sem,
    out_send,
    out_recv,
    back_send,
    back_recv,
    far_sem,
):
    n = n_sp * n_tp
    sp, tp = lax.axis_index("sp"), lax.axis_index("tp")
    me = sp * n_tp + tp
    rows, channels = value_ref.shape
    tokens, model = resid_ref.shape
    width = taps_ref.shape[0]
    group = glu_ext.shape[2]
    groups = channels // group

    near = n // 2
    far = flip(me, near)

    def place(index):
        return (index // n_tp, index % n_tp)

    loads = [
        pltpu.make_async_copy(a, b, w_sem.at[i])
        for i, (a, b) in enumerate(
            [
                (conv_out_hbm, conv_out),
                (sg_hbm, sg),
                (su_hbm, su),
                (sd_hbm, sd),
                (eg_hbm, eg),
                (eu_hbm, eu),
                (ed_hbm, ed),
            ]
        )
    ]
    for load in loads:
        load.start()

    barrier = pltpu.get_barrier_semaphore()
    for j in range(1, n):
        pl.semaphore_signal(barrier, inc=1, device_id=place(flip(me, j)), device_id_type=MESH_ID)

    glu = (value_ref[...].astype(F32) * jax.nn.sigmoid(gate_ref[...].astype(F32))).astype(BF16)
    halo_send[...] = glu[rows - HALO :, :]
    for g in range(groups):
        glu_ext[g, pl.ds(HALO, rows), :] = glu[:, g * group : (g + 1) * group].astype(F32)
    for at in range(0, rows, group):
        row = ids_ref[:, at : at + group].astype(F32)
        column = jnp.broadcast_to(row, (group, group)).T
        ids_here[pl.ds(at, group), :] = column
        ids_ext[pl.ds(HALO + at, group), :] = column
    tap_rows[pl.ds(0, width), :] = taps_ref[...].astype(F32)

    pl.semaphore_wait(barrier, n - 1)

    halo_copies = [
        pltpu.make_async_remote_copy(
            src_ref=halo_send,
            dst_ref=halo_recv,
            send_sem=halo_sem.at[0],
            recv_sem=halo_sem.at[1],
            device_id=(sp + 1, tp),
            device_id_type=MESH_ID,
        ),
        pltpu.make_async_remote_copy(
            src_ref=ids_here.at[pl.ds(rows - HALO, HALO)],
            dst_ref=ids_ext.at[pl.ds(0, HALO)],
            send_sem=halo_sem.at[2],
            recv_sem=halo_sem.at[3],
            device_id=(sp + 1, tp),
            device_id_type=MESH_ID,
        ),
    ]

    @pl.when(sp < n_sp - 1)
    def _():
        for copy in halo_copies:
            copy.start()

    @pl.when(sp == 0)
    def _():
        glu_ext[:, pl.ds(0, HALO), :] = jnp.zeros((groups, HALO, group), F32)
        ids_ext[pl.ds(0, HALO), :] = jnp.full((HALO, group), -1.0, F32)

    def to_far(src, dst, index):
        return pltpu.make_async_remote_copy(
            src_ref=src,
            dst_ref=dst,
            send_sem=far_sem.at[2 * index],
            recv_sem=far_sem.at[2 * index + 1],
            device_id=place(far),
            device_id_type=MESH_ID,
        )

    routes_copy = to_far(routes_ref, far_routes, 0)
    weight_copy = to_far(weight_ref, far_weight, 1)
    routes_copy.start()
    weight_copy.start()

    slots = near * capacity
    first = (me // near) * near
    tri_r = lax.broadcasted_iota(jnp.int32, (tokens, tokens), 0)
    tri_c = lax.broadcasted_iota(jnp.int32, (tokens, tokens), 1)
    later = (tri_r < tri_c).astype(F32).astype(BF16)
    spread_t = (
        (
            lax.broadcasted_iota(jnp.int32, (slots, near), 0) // capacity
            == lax.broadcasted_iota(jnp.int32, (slots, near), 1)
        )
        .astype(F32)
        .astype(BF16)
    )
    row_slot = (lax.broadcasted_iota(jnp.int32, (slots, tokens), 0) % capacity).astype(F32)
    row_expert = first + lax.broadcasted_iota(jnp.int32, (slots, tokens), 0) // capacity
    expert_row = first + lax.broadcasted_iota(jnp.int32, (near, tokens), 0)

    def tables(routes, weight):
        member = (
            (routes[0:1, :] == expert_row).astype(F32)
            + (routes[1:2, :] == expert_row).astype(F32)
        ).astype(BF16)
        slot = jnp.dot(member, later, preferred_element_type=F32).astype(BF16)
        right = jnp.dot(spread_t, slot, preferred_element_type=F32) == row_slot
        hit0 = jnp.where(right & (routes[0:1, :] == row_expert), 1.0, 0.0)
        hit1 = jnp.where(right & (routes[1:2, :] == row_expert), 1.0, 0.0)
        pick = (hit0 + hit1).astype(BF16)
        mix = (hit0 * weight[0:1, :] + hit1 * weight[1:2, :]).T
        high = mix.astype(BF16)
        return pick, high, (mix - high.astype(F32)).astype(BF16)

    pick, w_high, w_low = tables(routes_ref[...], weight_ref[...])

    @pl.when(sp > 0)
    def _():
        for copy in halo_copies:
            copy.wait_recv()
        for g in range(groups):
            glu_ext[g, pl.ds(0, HALO), :] = halo_recv[:, g * group : (g + 1) * group].astype(F32)

    @pl.when(sp < n_sp - 1)
    def _():
        for copy in halo_copies:
            copy.wait_send()

    def conv_block(start):
        def body(i, carry):
            r = pl.multiple_of(start + i * CHUNK, CHUNK)
            mine = ids_here[pl.ds(r, CHUNK), :]
            sums = [jnp.zeros((CHUNK, group), F32) for _ in range(groups)]
            for tap in range(width):
                off = HALO - width + 1 + tap
                same = ids_ext[pl.ds(r + off, CHUNK), :] == mine
                for g in range(groups):
                    term = (
                        tap_rows[tap : tap + 1, g * group : (g + 1) * group]
                        * glu_ext[g, pl.ds(r + off, CHUNK), :]
                    )
                    sums[g] = sums[g] + jnp.where(same, term, 0.0)
            for g in range(groups):
                cols = slice(g * group, (g + 1) * group)
                centered = sums[g] - jnp.mean(sums[g], axis=-1, keepdims=True)
                var = jnp.mean(centered * centered, axis=-1, keepdims=True)
                v = centered * lax.rsqrt(var + epsilon) * gain_ref[:, cols] + shift_ref[:, cols]
                act[pl.ds(r, CHUNK), cols] = silu(v).astype(BF16)
            return carry

        lax.fori_loop(0, tokens // CHUNK, body, 0)

    other = (tp + 1) % n_tp
    theirs = pl.multiple_of(other * tokens, tokens)
    mine_at = pl.multiple_of(tp * tokens, tokens)
    conv_block(theirs)
    act_copy = pltpu.make_async_remote_copy(
        src_ref=act.at[pl.ds(theirs, tokens)],
        dst_ref=act_recv,
        send_sem=act_sem.at[0],
        recv_sem=act_sem.at[1],
        device_id=(sp, other),
        device_id_type=MESH_ID,
    )
    act_copy.start()
    conv_block(mine_at)
    loads[0].wait()
    half = channels
    projected = jnp.dot(
        act[pl.ds(mine_at, tokens), :],
        conv_out[pl.ds(pl.multiple_of(tp * half, half), half), :],
        preferred_element_type=F32,
    )
    act_copy.wait()
    projected = projected + jnp.dot(
        act_recv[...],
        conv_out[pl.ds(pl.multiple_of(other * half, half), half), :],
        preferred_element_type=F32,
    )
    stream = (resid_ref[...].astype(F32) + projected).astype(BF16).astype(F32)
    base_ref[...] = stream
    normed = (
        stream
        * lax.rsqrt(jnp.mean(stream * stream, axis=-1, keepdims=True) + epsilon)
        * ngain_ref[...]
    ).astype(BF16)
    normed_ref[...] = normed

    per = near // 2
    block = per * capacity

    def piece(index):
        return pl.ds(pl.multiple_of(index * capacity, capacity), capacity)

    def exchange(src, dst, sems, index, peer):
        return pltpu.make_async_remote_copy(
            src_ref=src,
            dst_ref=dst,
            send_sem=sems[0].at[index],
            recv_sem=sems[1].at[index],
            device_id=place(peer),
            device_id_type=MESH_ID,
        )

    out_sems, back_sems = (out_send, out_recv), (back_send, back_recv)
    here = me % near

    def own_out(k):
        peer = flip(me, k)
        return exchange(send_own.at[piece(peer % near)], arrived.at[piece(me)], out_sems, k, peer)

    def far_out(k):
        peer = flip(me, k)
        return exchange(
            send_far.at[piece(peer % near)], arrived.at[piece(far)], out_sems, near + k, peer
        )

    def own_back(k):
        peer = flip(me, k)
        return exchange(result.at[piece(peer)], returned.at[piece(here)], back_sems, k, peer)

    def far_back(k):
        peer, source = flip(me, k), flip(me, near + k)
        return exchange(
            result.at[piece(source)], relayed.at[piece(here)], back_sems, near + k, peer
        )

    token_copy = to_far(normed_ref, far_tokens, 2)
    token_copy.start()
    send_own[...] = jnp.dot(pick, normed_ref[...], preferred_element_type=F32).astype(BF16)
    for k in range(near - 1, 0, -1):
        own_out(k).start()
    arrived[piece(me), :] = send_own[piece(here), :]
    routes_copy.wait()
    weight_copy.wait()
    far_pick, far_high, far_low = tables(far_routes[...], far_weight[...])

    for load in loads[1:4]:
        load.wait()
    shared = (
        silu(jnp.dot(normed_ref[...], sg[...], preferred_element_type=F32))
        * jnp.dot(normed_ref[...], su[...], preferred_element_type=F32)
    ).astype(BF16)
    base_ref[...] += jnp.dot(shared, sd[...], preferred_element_type=F32)
    for load in loads[4:]:
        load.wait()

    def experts(b):
        for low in range(per):
            j = b * per + low
            if j % near:
                (own_out(j) if j < near else far_out(j - near)).wait_recv()
        at = pl.ds(pl.multiple_of(flip(me // per, b) * block, block), block)
        x = arrived[at, :]
        hidden = (
            silu(jnp.dot(x, eg[0], preferred_element_type=F32))
            * jnp.dot(x, eu[0], preferred_element_type=F32)
        ).astype(BF16)
        result[at, :] = jnp.dot(hidden, ed[0], preferred_element_type=F32).astype(BF16)

    token_copy.wait_recv()
    send_far[...] = jnp.dot(far_pick, far_tokens[...], preferred_element_type=F32).astype(BF16)
    for k in range(near - 1, 0, -1):
        far_out(k).start()
    arrived[piece(far), :] = send_far[piece(here), :]

    experts(0)
    for k in range(per - 1, 0, -1):
        own_back(k).start()
    returned[piece(here), :] = result[piece(me), :]
    experts(1)
    experts(2)
    for k in range(per - 1, 0, -1):
        far_back(k).start()
    relayed[piece(here), :] = result[piece(far), :]
    experts(3)
    for k in range(near - 1, per - 1, -1):
        far_back(k).start()

    for k in range(1, near):
        far_back(k).wait_recv()
    back = relayed[...]
    part_send[...] = (
        jnp.dot(far_high, back, preferred_element_type=F32)
        + jnp.dot(far_low, back, preferred_element_type=F32)
    ).astype(BF16)
    part_copy = to_far(part_send, part_recv, 3)
    part_copy.start()
    for k in range(near - 1, per - 1, -1):
        own_back(k).start()

    for k in range(1, near):
        own_back(k).wait_recv()
    back = returned[...]
    base_ref[...] += jnp.dot(w_high, back, preferred_element_type=F32) + jnp.dot(
        w_low, back, preferred_element_type=F32
    )
    part_copy.wait_recv()
    out_ref[...] = (base_ref[...] + part_recv[...].astype(F32)).astype(BF16)
    for k in range(1, near):
        own_out(k).wait_send()
        far_out(k).wait_send()
        own_back(k).wait_send()
        far_back(k).wait_send()
    token_copy.wait_send()
    part_copy.wait_send()


def fused(
    conv_value,
    conv_gate,
    taps,
    doc_ids,
    gn_gain,
    gn_shift,
    conv_out,
    residual,
    norm_gain,
    routes,
    route_weight,
    expert_gate,
    expert_up,
    expert_down,
    shared_gate,
    shared_up,
    shared_down,
):
    n_sp, n_tp = lax.axis_size("sp"), lax.axis_size("tp")
    n = n_sp * n_tp
    rows, channels = conv_value.shape
    tokens, model = residual.shape
    capacity = 2 * tokens * routes.shape[1] // n
    group = channels * n_tp // GROUPS
    near_slots = n // 2 * capacity
    vmem = pl.BlockSpec(memory_space=pltpu.VMEM)
    hbm = pl.BlockSpec(memory_space=pl.ANY)
    dma = pltpu.SemaphoreType.DMA
    return pl.pallas_call(
        functools.partial(fused_kernel, n_sp, n_tp, capacity),
        out_shape=jax.ShapeDtypeStruct((tokens, model), BF16),
        in_specs=[vmem] * 10 + [hbm] * 7,
        out_specs=vmem,
        scratch_shapes=[
            pltpu.VMEM((channels // group, rows + HALO, group), F32),
            pltpu.VMEM((rows + HALO, group), F32),
            pltpu.VMEM((taps.shape[0] + 1, channels), F32),
            pltpu.VMEM((HALO, channels), BF16),
            pltpu.VMEM((HALO, channels), BF16),
            pltpu.VMEM((rows, channels), BF16),
            pltpu.VMEM((tokens, channels), BF16),
            pltpu.VMEM((tokens, model), BF16),
            pltpu.VMEM((tokens, model), F32),
            pltpu.VMEM((tokens, model), BF16),
            pltpu.VMEM((2, tokens), jnp.int32),
            pltpu.VMEM((2, tokens), F32),
            pltpu.VMEM((rows, group), F32),
            pltpu.VMEM((near_slots, model), BF16),
            pltpu.VMEM((near_slots, model), BF16),
            pltpu.VMEM((2 * near_slots, model), BF16),
            pltpu.VMEM((2 * near_slots, model), BF16),
            pltpu.VMEM((near_slots, model), BF16),
            pltpu.VMEM((near_slots, model), BF16),
            pltpu.VMEM((tokens, model), BF16),
            pltpu.VMEM((tokens, model), BF16),
            pltpu.VMEM(conv_out.shape, BF16),
            pltpu.VMEM(expert_gate.shape, BF16),
            pltpu.VMEM(expert_up.shape, BF16),
            pltpu.VMEM(expert_down.shape, BF16),
            pltpu.VMEM(shared_gate.shape, BF16),
            pltpu.VMEM(shared_up.shape, BF16),
            pltpu.VMEM(shared_down.shape, BF16),
            dma((7,)),
            dma((4,)),
            dma((2,)),
            dma((n,)),
            dma((n,)),
            dma((n,)),
            dma((n,)),
            dma((8,)),
        ],
        compiler_params=pltpu.CompilerParams(
            collective_id=0, has_side_effects=True, vmem_limit_bytes=VMEM_LIMIT
        ),
    )(
        conv_value,
        conv_gate,
        taps,
        doc_ids[None, :],
        gn_gain[None, :],
        gn_shift[None, :],
        residual,
        norm_gain[None, :],
        routes.T,
        route_weight.T,
        conv_out,
        expert_gate,
        expert_up,
        expert_down,
        shared_gate,
        shared_up,
        shared_down,
    )


VMEM_LIMIT = 58 * 1024 * 1024


def fits(mesh):
    n = mesh.size
    return n & (n - 1) == 0 and n <= 32 and mesh.shape["tp"] == 2


def solution(mesh):
    return jax.shard_map(
        fused if fits(mesh) else per_device,
        mesh=mesh,
        in_specs=(
            P("sp", "tp"),
            P("sp", "tp"),
            P(None, "tp"),
            P("sp"),
            P("tp"),
            P("tp"),
            P(),
            P(("sp", "tp"), None),
            P(),
            P(("sp", "tp"), None),
            P(("sp", "tp"), None),
            P(("sp", "tp"), None, None),
            P(("sp", "tp"), None, None),
            P(("sp", "tp"), None, None),
            P(),
            P(),
            P(),
        ),
        out_specs=P(("sp", "tp"), None),
        check_vma=False,
    )
```
